1024 devices in a mesh: sp: 256 (over z, y, core), tp: 4 (over x).
Axes of the slice: x: 4, y: 8, z: 16, core: 2. Of those that a mesh axis runs over, the one named last changes fastest.
Arguments:
- resid: bfloat16 [65536, 2048], P('sp', 'tp'), may hold values from -80 to 80, as said below
- norm_gain: float32 [2, 2048], P(None, 'tp'), may hold values from 0.1 to 1.9
- w_in: bfloat16 [2, 2048, 1024], P(None, 'tp', 'sp'), may hold values from -0.125 to 0.125
- w_pool: bfloat16 [2, 4, 256, 256], P(None, 'tp'), may hold values from -0.375 to 0.375
- pool_scale: float32 [2, 1024], P(None, 'tp'), may hold values from 0.1 to 1.9
- w_out: bfloat16 [2, 1024, 2048], P(None, 'sp', 'tp'), may hold values from -0.1875 to 0.1875
- final_gain: float32 [2048], P('tp'), may hold values from 0.1 to 1.9
Outputs:
- normed: bfloat16 [65536, 2048], P('sp', 'tp')
The draws below stay inside these ranges and needn't reach their ends.
Inputs may be any that keep to these rules, and one draw needn't show every extreme that they name: `resid`: Real-valued entries of order 0.1 to ten.
All inputs are finite; a program needn't handle non-finite values.
Results may differ from the reference program's by a relative error of at most 0.015.
Values may be sent and summed in bfloat16 or wider, within the bound.
No kernel may reach another device: no remote copies, remote signals or barrier semaphores. Data moves between devices by JAX's collectives and lax.ppermute only.
A program may use at most 32 MiB of HBM per device.

```python
import jax
import jax.numpy as jnp
from jax import lax

D = 2048
GROUPS = 4
CG = 256
LAYERS = 2
POOL = 1024
TOKENS = 65536
N_TP = 4


def draw_resid(key, part):
    keys = jax.random.split(jax.random.fold_in(key, 11), 3)
    row_scale = 10.0 ** jax.random.uniform(keys[0], (TOKENS, 1), jnp.float32, -0.5, 0.5)
    position = jnp.arange(D, dtype=jnp.float32) / D
    jitter = jnp.exp(jax.random.uniform(keys[1], (1, D), jnp.float32, -0.35, 0.35))
    col_scale = (10.0 ** (position - 0.5))[None, :] * jitter
    base = jnp.clip(jax.random.normal(keys[2], (TOKENS, D), jnp.float32), -4.0, 4.0)
    return (base * row_scale * col_scale).astype(jnp.bfloat16)


def block_levels(key, dims, cuts, least, top_value):
    def one(dim, shards_of):
        heights = jax.random.uniform(jax.random.fold_in(jax.random.fold_in(key, 6), dim), (shards_of,), jnp.float32, least / len(cuts), top_value / len(cuts))
        return jnp.repeat(jnp.exp(heights), dims[dim] // shards_of).reshape((-1,) + (1,) * (len(dims) - dim - 1))

    loudness = one(*cuts[0])
    for cut in cuts[1:]:
        loudness = loudness * one(*cut)
    return loudness


def scatter_about(stream_key, extent, spread, most, cuts=(), kind=jnp.bfloat16):
    factor_of = block_levels(stream_key, extent, cuts, -0.22, 0.18) if cuts else 1.0
    values = jax.random.normal(stream_key, extent, jnp.float32) * spread * factor_of
    return jnp.minimum(jnp.maximum(values, -most), most).astype(kind)


def setup_inputs(seed: int = 0) -> dict:
    seeds = jax.random.split(jax.random.key(seed), 8)
    resid = draw_resid(jax.random.fold_in(seeds[7], 71), 0)
    norm_gain = jnp.clip(1.0 + 0.18 * jax.random.normal(seeds[1], (LAYERS, D), jnp.float32), 0.1, 1.9)
    w_in = scatter_about(seeds[2], (LAYERS, D, POOL), D ** -0.5, 0.125, ((1, 4), (2, 256)))
    w_pool = scatter_about(seeds[3], (LAYERS, GROUPS, CG, CG), CG ** -0.5, 0.375, ((1, 4),))
    pool_scale = jnp.clip(1.0 + 0.18 * jax.random.normal(seeds[4], (LAYERS, POOL), jnp.float32), 0.1, 1.9)
    w_out = scatter_about(seeds[5], (LAYERS, POOL, D), POOL ** -0.5, 0.1875, ((1, 256), (2, 4)))
    final_gain = jnp.clip(1.0 + 0.18 * jax.random.normal(seeds[6], (D,), jnp.float32), 0.1, 1.9)
    return {"resid": resid, "norm_gain": norm_gain, "w_in": w_in, "w_pool": w_pool, "pool_scale": pool_scale, "w_out": w_out, "final_gain": final_gain}


margin = 8
eps = 1e-06

def nested_sums(padded, count_rows):
    total = padded[margin - 1:margin - 1 + count_rows] + padded[margin:margin + count_rows]
    sums = [total]
    for level in range(1, 4):
        half = 2 ** level
        for offset in range(half // 2 + 1, half + 1):
            total = total + padded[margin - offset:margin - offset + count_rows]
        for offset in range(half // 2, half):
            total = total + padded[margin + offset:margin + offset + count_rows]
        sums.append(total)
    return sums

def window_count(where, seq_len, level):
    left = 2 ** level
    right = 2 ** level - 1
    upper = jnp.clip(where + right + 1, 0, seq_len)
    lower = jnp.clip(where - left, 0, seq_len)
    return (upper - lower).astype(jnp.float32)

def scaled(xf, gain):
    squares = lax.optimization_barrier(jnp.sum(xf * xf, axis=1))
    return (xf * lax.rsqrt(squares / D + eps)[:, None] * gain[None, :]).astype(jnp.bfloat16)

def reference(resid, norm_gain, w_in, w_pool, pool_scale, w_out, final_gain):
    where = jnp.arange(TOKENS, dtype=jnp.int32)
    block = D // N_TP
    xf = resid.astype(jnp.float32)
    for layer in range(LAYERS):
        hidden = scaled(xf, norm_gain[layer])
        total = jnp.zeros((TOKENS, POOL), jnp.float32)
        for span_index in range(N_TP):
            part = jnp.dot(hidden[:, span_index * block:(span_index + 1) * block], w_in[layer, span_index * block:(span_index + 1) * block], preferred_element_type=jnp.float32).astype(jnp.bfloat16)
            part = lax.optimization_barrier(part)
            total = total + part.astype(jnp.float32)
        upward = total.astype(jnp.bfloat16)
        upward_f = upward.astype(jnp.float32)
        pieces = []
        for group in range(GROUPS):
            cols = upward_f[:, group * CG:(group + 1) * CG]
            padded = jnp.pad(cols, ((margin, margin), (0, 0)))
            wsum = nested_sums(padded, TOKENS)[group]
            counted = window_count(where, TOKENS, group)
            pooled = (wsum / counted[:, None] - cols).astype(jnp.bfloat16)
            mapped = jnp.dot(pooled, w_pool[layer, group], preferred_element_type=jnp.float32)
            pieces.append(mapped * pool_scale[layer, group * CG:(group + 1) * CG][None, :])
        mixed = jnp.concatenate(pieces, axis=1).astype(jnp.bfloat16)
        output = jnp.dot(mixed, w_out[layer], preferred_element_type=jnp.float32)
        stored = (xf + output).astype(jnp.bfloat16)
        stored = lax.optimization_barrier(stored)
        xf = stored.astype(jnp.float32)
    return scaled(xf, final_gain)
```

```python
import functools

import jax
import jax.numpy as jnp
from jax import lax
from jax.experimental import pallas as pl
from jax.experimental.pallas import tpu as pltpu
from jax.sharding import PartitionSpec as P


EPS = 1e-06
MARGIN = 8
Y, C = 8, 2
BF, F32 = jnp.bfloat16, jnp.float32
LIMIT = 16 * 2**20
ROWS = 16


def order_matrix(core, base, size):
    pos = lax.broadcasted_iota(jnp.int32, (size, size), 0)
    nat = lax.broadcasted_iota(jnp.int32, (size, size), 1)
    half = Y * 16
    y = (base + ((pos & (half - 1)) >> 4)) & (Y - 1)
    c = core ^ jnp.where(pos >= half, 1, 0)
    zr, r = (pos >> 2) & 3, pos & 3
    where = zr * (Y * C * 4) + y * (C * 4) + c * 4 + r
    return jnp.where(where == nat, 1.0, 0.0).astype(BF)


def dot_nt(a, b):
    return lax.dot_general(a, b, (((1,), (1,)), ((), ())), preferred_element_type=F32)


def dot_nn(a, b):
    return jnp.dot(a, b, preferred_element_type=F32)


def square_rows(xf):
    sq = xf * xf
    hi = sq.astype(BF)
    lo = (sq - hi.astype(F32)).astype(BF)
    ones = jnp.ones((ROWS, xf.shape[1]), BF)
    return dot_nt(ones, hi) + dot_nt(ones, lo)


def to_column(row, rows):
    return jnp.transpose(jnp.broadcast_to(row, (128, rows)))


def group_rows(picks, g):
    parts = []
    for ref, q in picks:
        block = ref[:, g] if q is None else ref[:, q, g]
        n, rows, d = block.shape
        parts.append(block.reshape(n * rows, d))
    return jnp.concatenate(parts, axis=0)


def project(xf, gain, picks, outs, first_group):
    rows = xf.shape[0]
    xs = (xf * gain).astype(BF)
    first, last = square_rows(xf[:256]), square_rows(xf[rows - 256 :])
    f_hi, l_hi = first.astype(BF).astype(F32), last.astype(BF).astype(F32)
    row = lax.broadcasted_iota(jnp.int32, first.shape, 0)
    extra = jnp.where(
        row == 0,
        f_hi,
        jnp.where(row == 1, first - f_hi, jnp.where(row == 2, l_hi, jnp.where(row == 3, last - l_hi, 0.0))),
    ).astype(BF)
    for d, out in enumerate(outs):
        g = (first_group + d) & (len(outs) - 1)
        out[:rows] = dot_nt(xs, group_rows(picks, g)).astype(BF)
        out[rows:] = extra


def first_kernel(info, prev, own, after, gain, in_own, in_other, *outs):
    xf = jnp.concatenate([prev[...].astype(F32), own[...].astype(F32), after[...].astype(F32)], axis=0)
    project(xf, gain[0:1], ((in_own, None), (in_other, None)), outs, info[0])


def pool_kernel(seq_len, width, halo, layer, copies, info, wp, scale, *refs):
    recv, out = refs[:-1], refs[-1]
    if len(recv) == 1:
        recv = [recv[0].at[k] for k in range(recv[0].shape[0])]
    size = recv[0].shape[1]
    rows = recv[0].shape[0] - ROWS
    keep = rows - 2 * MARGIN
    g, core, tok0 = info[0], info[1], info[2]
    total = recv[0][:rows].astype(F32)
    extra = recv[0][rows:].astype(F32)
    for ref in recv[1:]:
        total = total + ref[:rows].astype(F32)
        extra = extra + ref[rows:].astype(F32)
    first = to_column(extra[0:1] + extra[1:2], 256)
    last = to_column(extra[2:3] + extra[3:4], 256)
    ss = jnp.concatenate([first, last[512 - rows :]], axis=0) if rows > 256 else first
    r = lax.rsqrt(ss / width + EPS)
    uf = total * jnp.concatenate([r, r], axis=1)
    at = tok0 - halo + lax.broadcasted_iota(jnp.int32, (rows, size), 0)
    uf = jnp.where((at >= 0) & (at < seq_len), uf, 0.0)
    u = uf.astype(BF)
    left = jnp.left_shift(1, g)
    d = (
        lax.broadcasted_iota(jnp.int32, (keep, rows), 1)
        - lax.broadcasted_iota(jnp.int32, (keep, rows), 0)
        - MARGIN
    )
    band = jnp.where((d >= -left) & (d < left), 1.0, 0.0).astype(BF)
    wsum = dot_nn(band, u)
    here = tok0 - halo + MARGIN + lax.broadcasted_iota(jnp.int32, (keep, size), 0)
    upper = jnp.clip(here + left, 0, seq_len)
    lower = jnp.clip(here - left, 0, seq_len)
    count = jnp.maximum(upper - lower, 1).astype(F32)
    pooled = (wsum / count - u.astype(F32)[MARGIN : MARGIN + keep]).astype(BF)
    order = order_matrix(core, 0, size)
    inner = dot_nn(order, wp[layer, 0]).astype(BF)
    mixed = (dot_nn(pooled, inner) * scale[layer : layer + 1]).astype(BF)
    mixed = dot_nt(mixed, order).astype(BF)
    if copies is None:
        out[...] = mixed
    else:
        for k in range(copies):
            out[k] = mixed


def added(xf, mixed, picks):
    total = xf
    for g in range(mixed.shape[0]):
        total = total + dot_nn(mixed[g], group_rows(picks, g))
    return total.astype(BF)


def middle_kernel(out_q, in_q, prev, own, after, mixed, gain, w_own, w_other, x_out, pay):
    xf = jnp.concatenate(
        [prev[...].astype(F32)[8:], own[...].astype(F32), after[...].astype(F32)[:8]], axis=0
    )
    x = added(xf, mixed, ((w_own, out_q), (w_other, out_q)))
    x_out[...] = x
    outs = [pay.at[k] for k in range(pay.shape[0])]
    project(x.astype(F32), gain[1:2], ((w_own, in_q), (w_other, in_q)), outs, 0)


def last_kernel(out_q, x_in, mixed, w_own, w_other, x_out, squares):
    rows = mixed.shape[1]
    xf = x_in[...].astype(F32)[MARGIN : MARGIN + rows]
    x = added(xf, mixed, ((w_own, out_q), (w_other, out_q)))
    x_out[...] = x
    sums = square_rows(x.astype(F32))[:8]
    for k in range(squares.shape[0]):
        squares[k] = sums


def norm_kernel(width, x_in, squares, gain, out):
    total = squares[0, 0:1]
    for k in range(1, squares.shape[0]):
        total = total + squares[k, 0:1]
    rows, d = x_in.shape
    r = lax.rsqrt(to_column(total, rows) / width + EPS)
    r = jnp.concatenate([r] * (d // 128), axis=1)
    out[...] = (x_in[...].astype(F32) * r * gain[...]).astype(BF)


def call(kernel, shapes, *args, smem=0):
    spaces = [pltpu.SMEM if i < smem else pltpu.VMEM for i in range(len(args))]
    specs = [pl.BlockSpec(memory_space=space) for space in spaces]
    held = [
        a if space is pltpu.SMEM else pltpu.with_memory_space_constraint(a, space)
        for a, space in zip(args, spaces)
    ]
    params = pltpu.CompilerParams(vmem_limit_bytes=LIMIT)
    return pl.pallas_call(kernel, out_shape=shapes, in_specs=specs, compiler_params=params)(*held)


def to_all(value, axis, groups=None, count=None):
    count = lax.axis_size(axis) if count is None else count
    return lax.all_to_all(
        jnp.broadcast_to(value[None], (count, *value.shape)), axis, 0, 0, axis_index_groups=groups
    )


def shards(resid, norm_gain, w_in, w_pool, pool_scale, w_out, final_gain):
    tok = resid.shape[0]
    block = resid.shape[1]
    n_sp, n_tp = lax.axis_size("sp"), lax.axis_size("tp")
    width = n_tp * block
    seq_len = tok * n_sp
    nz = n_sp // (Y * C)
    size = w_pool.shape[2]
    sp, tp = lax.axis_index("sp"), lax.axis_index("tp")
    at = lambda z, y, c: ((z % nz) * Y + (y % Y)) * C + c
    places = [(z, y, c) for z in range(nz) for y in range(Y) for c in range(C)]
    z_rings = [[at(z, y, c) for z in range(nz)] for y in range(Y) for c in range(C)]
    y_rings = [[at(z, y, c) for y in range(Y)] for z in range(nz) for c in range(C)]
    swap = [(at(z, y, c), at(z, y, 1 - c)) for z, y, c in places]
    send_across = lambda v: lax.ppermute(v, "sp", swap)

    before = lax.ppermute(resid[tok - 2 * MARGIN :], "sp", [(i, i + 1) for i in range(n_sp - 1)])
    after = lax.ppermute(resid[: 2 * MARGIN], "sp", [(i + 1, i) for i in range(n_sp - 1)])

    turned = jnp.swapaxes(w_in, 1, 2)
    mine = jnp.stack([turned[0], w_out[0], turned[1], w_out[1]])
    along_z = to_all(mine, "sp", z_rings, nz)
    along_z = jnp.swapaxes(along_z, 0, 1).reshape(4, n_tp, nz // n_tp * 4, block)
    early, late, before, after = lax.optimization_barrier(
        (along_z[0], along_z[1:], before, after)
    )
    in_own = to_all(early, "sp", y_rings, Y)
    in_other = send_across(in_own)
    late, in_own = lax.optimization_barrier((late, in_own))
    own = to_all(late, "sp", y_rings, Y)
    other = send_across(own)

    info = jnp.stack([tp, sp & (C - 1), sp * tok]).astype(jnp.int32)
    wide, mid = tok + 4 * MARGIN, tok + 2 * MARGIN
    exchange = lambda v: lax.all_to_all(v, "tp", 0, 0, tiled=True)

    pay = call(
        first_kernel,
        [jax.ShapeDtypeStruct((wide + ROWS, size), BF)] * n_tp,
        info, before, resid, after, norm_gain, in_own, in_other, smem=1,
    )
    recv = [pay[0]]
    for d in (2, 1, 3):
        recv.append(lax.ppermute(pay[d], "tp", [(i, (i + d) % n_tp) for i in range(n_tp)]))
    mixed = call(
        functools.partial(pool_kernel, seq_len, width, 2 * MARGIN, 0, None),
        jax.ShapeDtypeStruct((mid, size), BF),
        info, w_pool, pool_scale, *recv, smem=1,
    )
    mixed = lax.all_gather(mixed, "tp")
    x, pay = call(
        functools.partial(middle_kernel, 0, 1),
        (
            jax.ShapeDtypeStruct((mid, block), BF),
            jax.ShapeDtypeStruct((n_tp, mid + ROWS, size), BF),
        ),
        before, resid, after, mixed, norm_gain, own, other,
    )
    recv = exchange(pay)
    mixed = call(
        functools.partial(pool_kernel, seq_len, width, MARGIN, 1, n_tp),
        jax.ShapeDtypeStruct((n_tp, tok, size), BF),
        info, w_pool, pool_scale, recv, smem=1,
    )
    mixed = exchange(mixed)
    x, squares = call(
        functools.partial(last_kernel, 2),
        (jax.ShapeDtypeStruct((tok, block), BF), jax.ShapeDtypeStruct((n_tp, 8, tok), F32)),
        x, mixed, own, other,
    )
    squares = exchange(squares)
    return call(
        functools.partial(norm_kernel, width),
        jax.ShapeDtypeStruct((tok, block), BF),
        x, squares, final_gain[None],
    )


def solution(mesh):
    placed = (
        P("sp", "tp"),
        P(None, "tp"),
        P(None, "tp", "sp"),
        P(None, "tp", None, None),
        P(None, "tp"),
        P(None, "sp", "tp"),
        P("tp"),
    )

    return jax.shard_map(
        shards, mesh=mesh, in_specs=placed, out_specs=P("sp", "tp"), check_vma=False
    )
```

```python
import functools

import jax
import jax.numpy as jnp
from jax import lax
from jax.experimental import pallas as pl
from jax.experimental.pallas import tpu as pltpu
from jax.sharding import PartitionSpec as P


EPS = 1e-06
MARGIN = 8
Y, C = 8, 2
BF, F32 = jnp.bfloat16, jnp.float32
LIMIT = 16 * 2**20
ROWS = 16


def order_matrix(core, base, size):
    pos = lax.broadcasted_iota(jnp.int32, (size, size), 0)
    nat = lax.broadcasted_iota(jnp.int32, (size, size), 1)
    half = Y * 16
    y = (base + ((pos & (half - 1)) >> 4)) & (Y - 1)
    c = core ^ jnp.where(pos >= half, 1, 0)
    zr, r = (pos >> 2) & 3, pos & 3
    where = zr * (Y * C * 4) + y * (C * 4) + c * 4 + r
    return jnp.where(where == nat, 1.0, 0.0).astype(BF)


def dot_nt(a, b):
    return lax.dot_general(a, b, (((1,), (1,)), ((), ())), preferred_element_type=F32)


def dot_nn(a, b):
    return jnp.dot(a, b, preferred_element_type=F32)


def square_rows(xf):
    sq = xf * xf
    hi = sq.astype(BF)
    lo = (sq - hi.astype(F32)).astype(BF)
    ones = jnp.ones((ROWS, xf.shape[1]), BF)
    return dot_nt(ones, hi) + dot_nt(ones, lo)


def to_column(row, rows):
    return jnp.transpose(jnp.broadcast_to(row, (128, rows)))


def group_rows(picks, g):
    parts = []
    for ref, base in picks:
        block = ref[:, base + g]
        n, rows, d = block.shape
        parts.append(block.reshape(n * rows, d))
    return jnp.concatenate(parts, axis=0)


def project(xf, gain, picks, outs, first_group):
    rows = xf.shape[0]
    xs = (xf * gain).astype(BF)
    first, last = square_rows(xf[:256]), square_rows(xf[rows - 256 :])
    f_hi, l_hi = first.astype(BF).astype(F32), last.astype(BF).astype(F32)
    row = lax.broadcasted_iota(jnp.int32, first.shape, 0)
    extra = jnp.where(
        row == 0,
        f_hi,
        jnp.where(row == 1, first - f_hi, jnp.where(row == 2, l_hi, jnp.where(row == 3, last - l_hi, 0.0))),
    ).astype(BF)
    for d, out in enumerate(outs):
        g = (first_group + d) & (len(outs) - 1)
        out[:rows] = dot_nt(xs, group_rows(picks, g)).astype(BF)
        out[rows:] = extra


def pack_kernel(w_in, w_out, out):
    parts = (w_in[0], w_out[0], w_in[1], w_out[1])
    rows = jnp.concatenate([p.astype(F32) for p in parts], axis=0).astype(BF)
    for k in range(out.shape[0]):
        out[k] = rows


def sorted_rows(pieces):
    nz, rows, d = pieces.shape
    n = nz * rows
    new = lax.broadcasted_iota(jnp.int32, (n, n), 0)
    old = lax.broadcasted_iota(jnp.int32, (n, n), 1)
    weight, z, r = new // (4 * nz), (new >> 2) & (nz - 1), new & 3
    order = jnp.where(old == z * rows + weight * 4 + r, 1.0, 0.0).astype(BF)
    done = dot_nn(order, pieces[...].reshape(n, d)).astype(BF)
    return done.reshape(4, 4, nz, d)


def early_kernel(pieces, out):
    done = sorted_rows(pieces)[0]
    for k in range(out.shape[0]):
        out[k] = done


def late_kernel(info, pieces, out):
    done = sorted_rows(pieces)
    half = jnp.where((info[3] & 1) == 0, done[3, :2].astype(F32), done[3, 2:].astype(F32)).astype(BF)
    for k in range(out.shape[0]):
        out[k, :4] = done[1]
        out[k, 4:8] = done[2]
        out[k, 8:] = half


def first_kernel(info, prev, own, after, gain, in_own, in_other, *outs):
    xf = jnp.concatenate([prev[...].astype(F32), own[...].astype(F32), after[...].astype(F32)], axis=0)
    project(xf, gain[0:1], ((in_own, 0), (in_other, 0)), outs, info[0])


def pool_kernel(seq_len, width, halo, layer, copies, info, wp, scale, *refs):
    recv, out = refs[:-1], refs[-1]
    if len(recv) == 1:
        recv = [recv[0].at[k] for k in range(recv[0].shape[0])]
    size = recv[0].shape[1]
    rows = recv[0].shape[0] - ROWS
    keep = rows - 2 * MARGIN
    g, core, tok0 = info[0], info[1], info[2]
    total = recv[0][:rows].astype(F32)
    extra = recv[0][rows:].astype(F32)
    for ref in recv[1:]:
        total = total + ref[:rows].astype(F32)
        extra = extra + ref[rows:].astype(F32)
    first = to_column(extra[0:1] + extra[1:2], 256)
    last = to_column(extra[2:3] + extra[3:4], 256)
    ss = jnp.concatenate([first, last[512 - rows :]], axis=0) if rows > 256 else first
    r = lax.rsqrt(ss / width + EPS)
    uf = total * jnp.concatenate([r, r], axis=1)
    at = tok0 - halo + lax.broadcasted_iota(jnp.int32, (rows, size), 0)
    uf = jnp.where((at >= 0) & (at < seq_len), uf, 0.0)
    u = uf.astype(BF)
    left = jnp.left_shift(1, g)
    d = (
        lax.broadcasted_iota(jnp.int32, (keep, rows), 1)
        - lax.broadcasted_iota(jnp.int32, (keep, rows), 0)
        - MARGIN
    )
    band = jnp.where((d >= -left) & (d < left), 1.0, 0.0).astype(BF)
    wsum = dot_nn(band, u)
    here = tok0 - halo + MARGIN + lax.broadcasted_iota(jnp.int32, (keep, size), 0)
    upper = jnp.clip(here + left, 0, seq_len)
    lower = jnp.clip(here - left, 0, seq_len)
    count = jnp.maximum(upper - lower, 1).astype(F32)
    pooled = (wsum / count - u.astype(F32)[MARGIN : MARGIN + keep]).astype(BF)
    order = order_matrix(core, 0, size)
    inner = dot_nn(order, wp[layer, 0]).astype(BF)
    mixed = (dot_nn(pooled, inner) * scale[layer : layer + 1]).astype(BF)
    mixed = dot_nt(mixed, order).astype(BF)
    if copies is None:
        out[...] = mixed
    else:
        for k in range(copies):
            out[k] = mixed


def middle_kernel(info, prev, own, after, m_0, m_1, m_2, m_3, gain, w_own, w_other, x_out, pay, half):
    xf = jnp.concatenate(
        [prev[...].astype(F32)[8:], own[...].astype(F32), after[...].astype(F32)[:8]], axis=0
    )
    total = xf
    for d, ref in enumerate((m_0, m_1, m_2, m_3)):
        g = (info[0] - d) & 3
        total = total + dot_nn(ref[...], group_rows(((w_own, 0), (w_other, 0)), g))
    x = total.astype(BF)
    x_out[...] = x
    half[0] = w_own[:, 8:]
    half[1] = w_other[:, 8:]
    outs = [pay.at[k] for k in range(pay.shape[0])]
    project(x.astype(F32), gain[1:2], ((w_own, 4), (w_other, 4)), outs, 0)


def last_kernel(info, x_in, mixed, half, other_half, x_out, squares):
    rows = mixed.shape[1]
    total = x_in[...].astype(F32)[MARGIN : MARGIN + rows]
    mine = (info[3] & 1) * 2
    for ref, first in ((half, mine), (other_half, 2 - mine)):
        for j in range(2):
            total = total + dot_nn(mixed[first + j], group_rows(((ref.at[0], 0), (ref.at[1], 0)), j))
    x = total.astype(BF)
    x_out[...] = x
    sums = square_rows(x.astype(F32))[:8]
    for k in range(squares.shape[0]):
        squares[k] = sums


def norm_kernel(width, x_in, squares, gain, out):
    total = squares[0, 0:1]
    for k in range(1, squares.shape[0]):
        total = total + squares[k, 0:1]
    rows, d = x_in.shape
    r = lax.rsqrt(to_column(total, rows) / width + EPS)
    r = jnp.concatenate([r] * (d // 128), axis=1)
    out[...] = (x_in[...].astype(F32) * r * gain[...]).astype(BF)


def call(kernel, shapes, *args, smem=0, near=True):
    spaces = [pltpu.SMEM if i < smem else pltpu.VMEM for i in range(len(args))]
    specs = [pl.BlockSpec(memory_space=space) for space in spaces]
    held = [
        a if space is pltpu.SMEM
        else pltpu.with_memory_space_constraint(a, space if near else pltpu.HBM)
        for a, space in zip(args, spaces)
    ]
    params = pltpu.CompilerParams(vmem_limit_bytes=LIMIT)
    return pl.pallas_call(kernel, out_shape=shapes, in_specs=specs, compiler_params=params)(*held)


def shards(resid, norm_gain, w_in, w_pool, pool_scale, w_out, final_gain):
    tok = resid.shape[0]
    block = resid.shape[1]
    n_sp, n_tp = lax.axis_size("sp"), lax.axis_size("tp")
    width = n_tp * block
    seq_len = tok * n_sp
    nz = n_sp // (Y * C)
    size = w_pool.shape[2]
    sp, tp = lax.axis_index("sp"), lax.axis_index("tp")
    at = lambda z, y, c: ((z % nz) * Y + (y % Y)) * C + c
    places = [(z, y, c) for z in range(nz) for y in range(Y) for c in range(C)]
    z_rings = [[at(z, y, c) for z in range(nz)] for y in range(Y) for c in range(C)]
    y_rings = [[at(z, y, c) for y in range(Y)] for z in range(nz) for c in range(C)]
    swap = [(at(z, y, c), at(z, y, 1 - c)) for z, y, c in places]
    send_across = lambda v: lax.ppermute(v, "sp", swap)

    before = lax.ppermute(resid[tok - 2 * MARGIN :], "sp", [(i, i + 1) for i in range(n_sp - 1)])
    after = lax.ppermute(resid[: 2 * MARGIN], "sp", [(i + 1, i) for i in range(n_sp - 1)])

    turned = jnp.swapaxes(w_in, 1, 2)
    packed = call(
        pack_kernel,
        jax.ShapeDtypeStruct((nz, 16, block), BF),
        turned, w_out, near=False,
    )
    along_z = lax.all_to_all(packed, "sp", 0, 0, axis_index_groups=z_rings)
    along_z, before, after = lax.optimization_barrier((along_z, before, after))
    info = jnp.stack([tp, sp & (C - 1), sp * tok, sp >> 4]).astype(jnp.int32)
    early = call(early_kernel, jax.ShapeDtypeStruct((Y, n_tp, 16, block), BF), along_z)
    late = call(
        late_kernel,
        jax.ShapeDtypeStruct((Y, 10, 16, block), BF),
        info, along_z, smem=1,
    )
    in_own = lax.all_to_all(early, "sp", 0, 0, axis_index_groups=y_rings)
    in_other = send_across(in_own)
    late, in_own = lax.optimization_barrier((late, in_own))
    own = lax.all_to_all(late, "sp", 0, 0, axis_index_groups=y_rings)
    other = send_across(own)

    wide, mid = tok + 4 * MARGIN, tok + 2 * MARGIN
    exchange = lambda v: lax.all_to_all(v, "tp", 0, 0, tiled=True)

    pay = call(
        first_kernel,
        [jax.ShapeDtypeStruct((wide + ROWS, size), BF)] * n_tp,
        info, before, resid, after, norm_gain, in_own, in_other, smem=1,
    )
    recv = [pay[0]]
    for d in (2, 1, 3):
        recv.append(lax.ppermute(pay[d], "tp", [(i, (i + d) % n_tp) for i in range(n_tp)]))
    mixed = call(
        functools.partial(pool_kernel, seq_len, width, 2 * MARGIN, 0, None),
        jax.ShapeDtypeStruct((mid, size), BF),
        info, w_pool, pool_scale, *recv, smem=1,
    )
    parts = {0: mixed}
    for d in (2, 1, 3):
        parts[d] = lax.ppermute(mixed, "tp", [(i, (i + d) % n_tp) for i in range(n_tp)])
    x, pay, half = call(
        middle_kernel,
        (
            jax.ShapeDtypeStruct((mid, block), BF),
            jax.ShapeDtypeStruct((n_tp, mid + ROWS, size), BF),
            jax.ShapeDtypeStruct((2, Y, 2, 16, block), BF),
        ),
        info, before, resid, after, *(parts[d] for d in range(4)), norm_gain, own, other,
        smem=1,
    )
    other_half = lax.ppermute(half, "sp", [(at(z, y, c), at(z ^ 1, y, c)) for z, y, c in places])
    recv = exchange(pay)
    mixed = call(
        functools.partial(pool_kernel, seq_len, width, MARGIN, 1, n_tp),
        jax.ShapeDtypeStruct((n_tp, tok, size), BF),
        info, w_pool, pool_scale, recv, smem=1,
    )
    mixed = exchange(mixed)
    x, squares = call(
        last_kernel,
        (jax.ShapeDtypeStruct((tok, block), BF), jax.ShapeDtypeStruct((n_tp, 8, tok), F32)),
        info, x, mixed, half, other_half, smem=1,
    )
    squares = exchange(squares)
    return call(
        functools.partial(norm_kernel, width),
        jax.ShapeDtypeStruct((tok, block), BF),
        x, squares, final_gain[None],
    )


def solution(mesh):
    placed = (
        P("sp", "tp"),
        P(None, "tp"),
        P(None, "tp", "sp"),
        P(None, "tp", None, None),
        P(None, "tp"),
        P(None, "sp", "tp"),
        P("tp"),
    )

    return jax.shard_map(shards, mesh=mesh, in_specs=placed, out_specs=P("sp", "tp"), check_vma=False)
```

```python
import functools

import jax
import jax.numpy as jnp
from jax import lax
from jax.experimental import pallas as pl
from jax.experimental.pallas import tpu as pltpu
from jax.sharding import PartitionSpec as P


EPS = 1e-06
MARGIN = 8
Y, C = 8, 2
BF, F32 = jnp.bfloat16, jnp.float32
LIMIT = 16 * 2**20
ROWS = 16


def order_matrix(core, base, size):
    pos = lax.broadcasted_iota(jnp.int32, (size, size), 0)
    nat = lax.broadcasted_iota(jnp.int32, (size, size), 1)
    half = Y * 16
    y = (base + ((pos & (half - 1)) >> 4)) & (Y - 1)
    c = core ^ jnp.where(pos >= half, 1, 0)
    zr, r = (pos >> 2) & 3, pos & 3
    where = zr * (Y * C * 4) + y * (C * 4) + c * 4 + r
    return jnp.where(where == nat, 1.0, 0.0).astype(BF)


def dot_nt(a, b):
    return lax.dot_general(a, b, (((1,), (1,)), ((), ())), preferred_element_type=F32)


def dot_nn(a, b):
    return jnp.dot(a, b, preferred_element_type=F32)


def square_rows(xf):
    sq = xf * xf
    hi = sq.astype(BF)
    lo = (sq - hi.astype(F32)).astype(BF)
    ones = jnp.ones((ROWS, xf.shape[1]), BF)
    return dot_nt(ones, hi) + dot_nt(ones, lo)


def to_column(row, rows):
    return jnp.transpose(jnp.broadcast_to(row, (128, rows)))


def group_rows(picks, g):
    parts = []
    for ref, base in picks:
        block = ref[:, base + g]
        n, rows, d = block.shape
        parts.append(block.reshape(n * rows, d))
    return jnp.concatenate(parts, axis=0)


def project(xf, gain, picks, outs, first_group):
    rows = xf.shape[0]
    xs = (xf * gain).astype(BF)
    first, last = square_rows(xf[:256]), square_rows(xf[rows - 256 :])
    f_hi, l_hi = first.astype(BF).astype(F32), last.astype(BF).astype(F32)
    row = lax.broadcasted_iota(jnp.int32, first.shape, 0)
    extra = jnp.where(
        row == 0,
        f_hi,
        jnp.where(row == 1, first - f_hi, jnp.where(row == 2, l_hi, jnp.where(row == 3, last - l_hi, 0.0))),
    ).astype(BF)
    for d, out in enumerate(outs):
        g = (first_group + d) & (len(outs) - 1)
        out[:rows] = dot_nt(xs, group_rows(picks, g)).astype(BF)
        out[rows:] = extra


def pack_kernel(w_in, w_out, out):
    parts = (w_in[0], w_out[0], w_in[1], w_out[1])
    rows = jnp.concatenate([p.astype(F32) for p in parts], axis=0).astype(BF)
    for k in range(out.shape[0]):
        out[k] = rows


def sorted_rows(pieces, first, count):
    nz, rows, d = pieces.shape
    shape = (count * 4 * nz, nz * rows)
    new = lax.broadcasted_iota(jnp.int32, shape, 0)
    old = lax.broadcasted_iota(jnp.int32, shape, 1)
    weight, z, r = first + jnp.right_shift(new, (4 * nz).bit_length() - 1), (new >> 2) & (nz - 1), new & 3
    order = jnp.where(old == z * rows + weight * 4 + r, 1.0, 0.0).astype(BF)
    done = dot_nn(order, pieces[...].reshape(nz * rows, d)).astype(BF)
    return done.reshape(count, 4, nz, d)


def early_kernel(pieces, out):
    done = sorted_rows(pieces, 0, 1)[0]
    for k in range(out.shape[0]):
        out[k] = done


def late_kernel(info, pieces, out):
    done = sorted_rows(pieces, 1, 3)
    half = jnp.where((info[3] & 1) == 0, done[2, :2].astype(F32), done[2, 2:].astype(F32)).astype(BF)
    for k in range(out.shape[0]):
        out[k, :4] = done[0]
        out[k, 4:8] = done[1]
        out[k, 8:] = half


def first_kernel(info, prev, own, after, gain, in_own, in_other, *outs):
    xf = jnp.concatenate([prev[...].astype(F32), own[...].astype(F32), after[...].astype(F32)], axis=0)
    project(xf, gain[0:1], ((in_own, 0), (in_other, 0)), outs, info[0])


def pool_kernel(seq_len, width, halo, layer, copies, info, wp, scale, *refs):
    recv, out = refs[:-1], refs[-1]
    if len(recv) == 1:
        recv = [recv[0].at[k] for k in range(recv[0].shape[0])]
    size = recv[0].shape[1]
    rows = recv[0].shape[0] - ROWS
    keep = rows - 2 * MARGIN
    g, core, tok0 = info[0], info[1], info[2]
    total = recv[0][:rows].astype(F32)
    extra = recv[0][rows:].astype(F32)
    for ref in recv[1:]:
        total = total + ref[:rows].astype(F32)
        extra = extra + ref[rows:].astype(F32)
    first = to_column(extra[0:1] + extra[1:2], 256)
    last = to_column(extra[2:3] + extra[3:4], 256)
    ss = jnp.concatenate([first, last[512 - rows :]], axis=0) if rows > 256 else first
    r = lax.rsqrt(ss / width + EPS)
    uf = total * jnp.concatenate([r, r], axis=1)
    at = tok0 - halo + lax.broadcasted_iota(jnp.int32, (rows, size), 0)
    uf = jnp.where((at >= 0) & (at < seq_len), uf, 0.0)
    u = uf.astype(BF)
    left = jnp.left_shift(1, g)
    d = (
        lax.broadcasted_iota(jnp.int32, (keep, rows), 1)
        - lax.broadcasted_iota(jnp.int32, (keep, rows), 0)
        - MARGIN
    )
    band = jnp.where((d >= -left) & (d < left), 1.0, 0.0).astype(BF)
    wsum = dot_nn(band, u)
    here = tok0 - halo + MARGIN + lax.broadcasted_iota(jnp.int32, (keep, size), 0)
    upper = jnp.clip(here + left, 0, seq_len)
    lower = jnp.clip(here - left, 0, seq_len)
    count = jnp.maximum(upper - lower, 1).astype(F32)
    pooled = (wsum / count - u.astype(F32)[MARGIN : MARGIN + keep]).astype(BF)
    order = order_matrix(core, 0, size)
    inner = dot_nn(order, wp[layer, 0]).astype(BF)
    mixed = (dot_nn(pooled, inner) * scale[layer : layer + 1]).astype(BF)
    mixed = dot_nt(mixed, order).astype(BF)
    if copies is None:
        out[...] = mixed
    else:
        for k in range(copies):
            out[k] = mixed


def middle_kernel(info, prev, own, after, m_0, m_1, m_2, m_3, gain, w_own, w_other, x_out, pay, half):
    xf = jnp.concatenate(
        [prev[...].astype(F32)[8:], own[...].astype(F32), after[...].astype(F32)[:8]], axis=0
    )
    total = xf
    for d, ref in enumerate((m_0, m_1, m_2, m_3)):
        g = (info[0] - d) & 3
        total = total + dot_nn(ref[...], group_rows(((w_own, 0), (w_other, 0)), g))
    x = total.astype(BF)
    x_out[...] = x
    half[0] = w_own[:, 8:]
    half[1] = w_other[:, 8:]
    outs = [pay.at[k] for k in range(pay.shape[0])]
    project(x.astype(F32), gain[1:2], ((w_own, 4), (w_other, 4)), outs, 0)


def last_kernel(info, x_in, mixed, half, other_half, x_out, squares):
    rows = mixed.shape[1]
    total = x_in[...].astype(F32)[MARGIN : MARGIN + rows]
    mine = (info[3] & 1) * 2
    for ref, first in ((half, mine), (other_half, 2 - mine)):
        for j in range(2):
            total = total + dot_nn(mixed[first + j], group_rows(((ref.at[0], 0), (ref.at[1], 0)), j))
    x = total.astype(BF)
    x_out[...] = x
    sums = square_rows(x.astype(F32))[:8]
    for k in range(squares.shape[0]):
        squares[k] = sums


def norm_kernel(width, x_in, squares, gain, out):
    total = squares[0, 0:1]
    for k in range(1, squares.shape[0]):
        total = total + squares[k, 0:1]
    rows, d = x_in.shape
    r = lax.rsqrt(to_column(total, rows) / width + EPS)
    r = jnp.concatenate([r] * (d // 128), axis=1)
    out[...] = (x_in[...].astype(F32) * r * gain[...]).astype(BF)


def call(kernel, shapes, *args, smem=0, near=True):
    spaces = [pltpu.SMEM if i < smem else pltpu.VMEM for i in range(len(args))]
    specs = [pl.BlockSpec(memory_space=space) for space in spaces]
    held = [
        a if space is pltpu.SMEM
        else pltpu.with_memory_space_constraint(a, space if near else pltpu.HBM)
        for a, space in zip(args, spaces)
    ]
    params = pltpu.CompilerParams(vmem_limit_bytes=LIMIT)
    return pl.pallas_call(kernel, out_shape=shapes, in_specs=specs, compiler_params=params)(*held)


def shards(resid, norm_gain, w_in, w_pool, pool_scale, w_out, final_gain):
    tok = resid.shape[0]
    block = resid.shape[1]
    n_sp, n_tp = lax.axis_size("sp"), lax.axis_size("tp")
    width = n_tp * block
    seq_len = tok * n_sp
    nz = n_sp // (Y * C)
    size = w_pool.shape[2]
    sp, tp = lax.axis_index("sp"), lax.axis_index("tp")
    at = lambda z, y, c: ((z % nz) * Y + (y % Y)) * C + c
    places = [(z, y, c) for z in range(nz) for y in range(Y) for c in range(C)]
    z_rings = [[at(z, y, c) for z in range(nz)] for y in range(Y) for c in range(C)]
    y_rings = [[at(z, y, c) for y in range(Y)] for z in range(nz) for c in range(C)]
    swap = [(at(z, y, c), at(z, y, 1 - c)) for z, y, c in places]
    send_across = lambda v: lax.ppermute(v, "sp", swap)

    before = lax.ppermute(resid[tok - 2 * MARGIN :], "sp", [(i, i + 1) for i in range(n_sp - 1)])
    after = lax.ppermute(resid[: 2 * MARGIN], "sp", [(i + 1, i) for i in range(n_sp - 1)])

    turned = jnp.swapaxes(w_in, 1, 2)
    packed = call(
        pack_kernel,
        jax.ShapeDtypeStruct((nz, 16, block), BF),
        turned, w_out, near=False,
    )
    along_z = lax.all_to_all(packed, "sp", 0, 0, axis_index_groups=z_rings)
    along_z, before, after = lax.optimization_barrier((along_z, before, after))
    info = jnp.stack([tp, sp & (C - 1), sp * tok, sp >> 4]).astype(jnp.int32)
    early = call(early_kernel, jax.ShapeDtypeStruct((Y, n_tp, 16, block), BF), along_z)
    late = call(
        late_kernel,
        jax.ShapeDtypeStruct((Y, 10, 16, block), BF),
        info, along_z, smem=1,
    )
    in_own = lax.all_to_all(early, "sp", 0, 0, axis_index_groups=y_rings)
    in_other = send_across(in_own)
    late, in_own = lax.optimization_barrier((late, in_own))
    own = lax.all_to_all(late, "sp", 0, 0, axis_index_groups=y_rings)
    other = send_across(own)

    wide, mid = tok + 4 * MARGIN, tok + 2 * MARGIN
    exchange = lambda v: lax.all_to_all(v, "tp", 0, 0, tiled=True)

    pay = call(
        first_kernel,
        [jax.ShapeDtypeStruct((wide + ROWS, size), BF)] * n_tp,
        info, before, resid, after, norm_gain, in_own, in_other, smem=1,
    )
    recv = [pay[0]]
    for d in (2, 1, 3):
        recv.append(lax.ppermute(pay[d], "tp", [(i, (i + d) % n_tp) for i in range(n_tp)]))
    mixed = call(
        functools.partial(pool_kernel, seq_len, width, 2 * MARGIN, 0, None),
        jax.ShapeDtypeStruct((mid, size), BF),
        info, w_pool, pool_scale, *recv, smem=1,
    )
    parts = {0: mixed}
    for d in (2, 1, 3):
        parts[d] = lax.ppermute(mixed, "tp", [(i, (i + d) % n_tp) for i in range(n_tp)])
    x, pay, half = call(
        middle_kernel,
        (
            jax.ShapeDtypeStruct((mid, block), BF),
            jax.ShapeDtypeStruct((n_tp, mid + ROWS, size), BF),
            jax.ShapeDtypeStruct((2, Y, 2, 16, block), BF),
        ),
        info, before, resid, after, *(parts[d] for d in range(4)), norm_gain, own, other,
        smem=1,
    )
    other_half = lax.ppermute(half, "sp", [(at(z, y, c), at(z ^ 1, y, c)) for z, y, c in places])
    recv = exchange(pay)
    mixed = call(
        functools.partial(pool_kernel, seq_len, width, MARGIN, 1, n_tp),
        jax.ShapeDtypeStruct((n_tp, tok, size), BF),
        info, w_pool, pool_scale, recv, smem=1,
    )
    mixed = exchange(mixed)
    x, squares = call(
        last_kernel,
        (jax.ShapeDtypeStruct((tok, block), BF), jax.ShapeDtypeStruct((n_tp, 8, tok), F32)),
        info, x, mixed, half, other_half, smem=1,
    )
    squares = exchange(squares)
    return call(
        functools.partial(norm_kernel, width),
        jax.ShapeDtypeStruct((tok, block), BF),
        x, squares, final_gain[None],
    )


def solution(mesh):
    placed = (
        P("sp", "tp"),
        P(None, "tp"),
        P(None, "tp", "sp"),
        P(None, "tp", None, None),
        P(None, "tp"),
        P(None, "sp", "tp"),
        P("tp"),
    )

    return jax.shard_map(shards, mesh=mesh, in_specs=placed, out_specs=P("sp", "tp"), check_vma=False)
```
